32 devices in a mesh: grp: 2 (over x), ep: 16 (over z, y, core).
Axes of the slice: x: 2, y: 2, z: 4, core: 2. Of those that a mesh axis runs over, the one named last changes fastest.
Arguments:
- tokens_in: bfloat16 [64, 4096], P(('grp', 'ep')), parts along dimension 0, may hold values from -6 to 6
- mix_gain: float32 [4096], replicated, may hold values from 0.1 to 1.9
- w_gate_z: bfloat16 [4096, 4096], P(None, 'ep'), may hold values from -0.09375 to 0.09375
- w_value: bfloat16 [4096, 4096], P(None, 'ep'), may hold values from -0.09375 to 0.09375
- w_in_bc: bfloat16 [4096, 1024], P(None, 'ep'), may hold values from -0.09375 to 0.09375
- w_step: bfloat16 [4096, 64], replicated, may hold values from -0.09375 to 0.09375
- step_bias: float32 [64], replicated, may hold values from -4 to 0.5
- decay_log: float32 [64], replicated, may hold values from -1.5 to 2
- skip_gain: float32 [64], replicated, may hold values from 0.3 to 1.7
- conv_x_weight: float32 [4, 4096], replicated, may hold values from -3 to 3
- conv_bc_weight: float32 [4, 1024], replicated, may hold values from -3 to 3
- conv_x_state: bfloat16 [64, 3, 4096], P(('grp', 'ep')), parts along dimension 0, may hold values from -6 to 6
- conv_bc_state: bfloat16 [64, 3, 1024], P(('grp', 'ep')), parts along dimension 0, may hold values from -6 to 6
- ssm_state: float32 [64, 64, 64, 128], P(('grp', 'ep')), parts along dimension 0, may hold values from -3 to 3
- inner_gain: float32 [4096], replicated, may hold values from 0.1 to 1.9
- out_weight: bfloat16 [4096, 4096], P(None, 'ep'), may hold values from -0.09375 to 0.09375
- ffn_gain: float32 [4096], replicated, may hold values from 0.1 to 1.9
- expert_gate: bfloat16 [16, 4096, 512], P('ep'), may hold values from -0.09375 to 0.09375
- expert_up: bfloat16 [16, 4096, 512], P('ep'), may hold values from -0.09375 to 0.09375
- expert_down: bfloat16 [16, 512, 4096], P('ep'), may hold values from -0.25 to 0.25
- routes: int32 [64, 4], P(('grp', 'ep')), parts along dimension 0, may hold values from 0 to 15, all different within a row; in each aligned block of 2 rows (0 to 1, 2 to 3, ...) at most 2 rows name the same one
- route_weight: float32 [64, 4], P(('grp', 'ep')), parts along dimension 0, may hold values from 0.1 to 1
Outputs:
- out_tokens: bfloat16 [64, 4096], P(('grp', 'ep')), parts along dimension 0
- new_state: float32 [64, 64, 64, 128], P(('grp', 'ep')), parts along dimension 0
- new_conv_x: bfloat16 [64, 3, 4096], P(('grp', 'ep')), parts along dimension 0
- new_conv_bc: bfloat16 [64, 3, 1024], P(('grp', 'ep')), parts along dimension 0
The draws below stay inside these ranges and needn't reach their ends.
There are 2 independent parts, one for each index of `grp`. The reference program is written for one: setup_inputs(seed, part) draws one part's arguments, and reference() takes and returns one part's arrays. A program takes and returns all parts, laid end to end along the dimension named above; an argument that names none is the same for every part. Nothing has to cross between parts.
Inputs may be any that keep to these rules, and one draw needn't show every extreme that they name: `routes`: each row names 4 different experts. Among the rows of one device no expert is named more than 2 times, and some device names some expert exactly 2 times.
All inputs are finite; a program needn't handle non-finite values.
Results may differ from the reference program's by a relative error of at most 0.015.
Values may be sent and summed in bfloat16 or wider, within the bound.
A program may use at most 64 MiB of HBM per device.

```python
import math
import jax
import jax.numpy as jnp
import numpy as np
from jax import lax

D = 4096
HEADS = 64
HEAD_DIM = 64
GROUPS = 4
NSTATE = 128
CONV = 4
FF = 512
TOPK = 4
SLOT = 2
SEQ_DEV = 2
INNER = 4096
EXPERTS = 16
BATCH = 32


def block_levels(key, dims, shards, least, high):
    level, own = 1.0, jax.random.fold_in(key, 6)
    for position, blocks in shards:
        heights = jnp.exp(jax.random.uniform(jax.random.fold_in(own, position), (blocks,), jnp.float32, least / len(shards), high / len(shards)))
        level = level * jnp.repeat(heights, dims[position] // blocks).reshape([-1 if axis == position else 1 for axis in range(len(dims))])
    return level


def assign_block(rng, own, number, rows, amount, top, bound, lean):
    sequence = jax.random.permutation(rng, amount)
    crowded, common = shares(amount, rows * top, bound, lean, True), shares(amount, rows * top, bound, lean, False)
    places = jnp.arange(amount)

    def named(sizes, rotation):
        used = int((sizes > 0).sum())
        fixed = max(1, used // 4)
        shifted = fixed + (places - fixed + rotation * (used - fixed)) % max(1, amount - fixed)
        return jnp.zeros((amount,), jnp.int32).at[sequence[jnp.where(places < fixed, places, shifted)]].set(jnp.asarray(sizes, jnp.int32))

    sizes = jnp.where(number % 4 == 0, named(crowded, number // 4), named(common, number - number // 4 - 1))
    mixed = jax.random.permutation(jax.random.fold_in(own, 3), amount)
    donor, receiver = mixed[0:amount // 2 * 2:2], mixed[1:amount // 2 * 2:2]
    margin = jnp.minimum(sizes[donor] - 1, bound - sizes[receiver]) // 2
    margin = jnp.where((donor == sequence[0]) | (receiver == sequence[0]) | (sizes[receiver] == 0), 0, jnp.maximum(margin, 0))
    shifted = jax.random.randint(jax.random.fold_in(own, 4), (amount // 2,), 0, 1 << 20) % (margin + 1)
    sizes = sizes.at[donor].add(-shifted).at[receiver].add(shifted)
    members = jnp.searchsorted(jnp.cumsum(sizes), jnp.arange(rows * top), side="right").astype(jnp.int32)
    table = members.reshape(top, rows).T
    table = table[jax.random.permutation(jax.random.fold_in(own, 1), rows)]
    rotation = jax.random.randint(jax.random.fold_in(own, 2), (rows, 1), 0, top)
    return jnp.take_along_axis(table, (jnp.arange(top)[None, :] + rotation) % top, axis=1)


def shares(amount, total, bound, lean, full):
    loads = [(1 << 20) // math.isqrt(rank ** lean) + 1 for rank in range(1, amount + 1)]
    largest = bound if full else min(bound, max(-(-total // amount), total * loads[0] // sum(loads)))
    least = 1 if total - largest >= amount - 1 else 0
    given, surplus = [largest] + [least] * (amount - 1), total - largest - least * (amount - 1)
    while surplus > 0:
        free = [i for i in range(1, amount) if given[i] < largest] or [i for i in range(1, amount) if given[i] < bound]
        pool, remaining = sum([loads[i] for i in free]), surplus
        for i in free:
            extra = min(bound - given[i], max(1, remaining * loads[i] // pool), surplus)
            given[i] = given[i] + extra
            surplus = surplus - extra
    return np.array(given)


def normal_values(own_key, shape, deviation, most, pieces=(), kind=jnp.bfloat16):
    array = jax.random.normal(own_key, shape, jnp.float32) * deviation
    if len(pieces) > 0:
        array = block_levels(own_key, shape, pieces, -0.22, 0.18) * array
    return jnp.clip(array, min=-most, max=most).astype(kind)


def setup_inputs(seed: int = 0, part: int = 0) -> dict:
    key_of = jax.random.split(jax.random.key(seed), 23)
    own_keys = jax.random.split(jax.random.fold_in(key_of[22], part), 23)
    tokens_in = normal_values(own_keys[0], (BATCH, D), 1.0, 6.0, ((0, 16),))
    mix_gain = jnp.clip(1.0 + 0.18 * jax.random.normal(key_of[1], (D,), jnp.float32), 0.1, 1.9)
    w_gate_z = normal_values(key_of[2], (D, INNER), D ** -0.5, 0.09375, ((1, 16),))
    w_value = normal_values(key_of[3], (D, INNER), D ** -0.5, 0.09375, ((1, 16),))
    w_in_bc = normal_values(key_of[4], (D, 2 * GROUPS * NSTATE), D ** -0.5, 0.09375, ((1, 16),))
    w_step = normal_values(key_of[5], (D, HEADS), D ** -0.5, 0.09375)
    step_bias = jnp.clip(jax.random.uniform(key_of[6], (HEADS,), jnp.float32, -4.0, 0.5), -4.0, 0.5)
    decay_log = jnp.clip(jax.random.uniform(key_of[7], (HEADS,), jnp.float32, -1.5, 2.0), -1.5, 2.0)
    skip_gain = jnp.clip(jax.random.uniform(key_of[8], (HEADS,), jnp.float32, 0.3, 1.7), 0.3, 1.7)
    conv_x_weight = normal_values(key_of[9], (CONV, INNER), 0.5, 3.0, (), jnp.float32)
    conv_bc_weight = normal_values(key_of[10], (CONV, 2 * GROUPS * NSTATE), 0.5, 3.0, (), jnp.float32)
    conv_x_state = normal_values(own_keys[11], (BATCH, CONV - 1, INNER), 1.0, 6.0, ((0, 16),))
    conv_bc_state = normal_values(own_keys[12], (BATCH, CONV - 1, 2 * GROUPS * NSTATE), 1.0, 6.0, ((0, 16),))
    ssm_state = normal_values(own_keys[13], (BATCH, HEADS, HEAD_DIM, NSTATE), 0.3, 3.0, ((0, 16),), jnp.float32)
    inner_gain = jnp.clip(1.0 + 0.18 * jax.random.normal(key_of[14], (INNER,), jnp.float32), 0.1, 1.9)
    out_weight = normal_values(key_of[15], (INNER, D), INNER ** -0.5, 0.09375, ((1, 16),))
    ffn_gain = jnp.clip(1.0 + 0.18 * jax.random.normal(key_of[16], (D,), jnp.float32), 0.1, 1.9)
    expert_gate = normal_values(key_of[17], (EXPERTS, D, FF), D ** -0.5, 0.09375, ((0, 16),))
    expert_up = normal_values(key_of[18], (EXPERTS, D, FF), D ** -0.5, 0.09375, ((0, 16),))
    expert_down = normal_values(key_of[19], (EXPERTS, FF, D), FF ** -0.5, 0.25, ((0, 16),))
    routes_keys = jax.random.split(jax.random.fold_in(own_keys[20], 1), BATCH // SEQ_DEV)
    routes_turns = jax.random.permutation(jax.random.fold_in(own_keys[20], 3), BATCH // SEQ_DEV)
    routes = jax.vmap(lambda own, number: assign_block(jax.random.fold_in(own_keys[20], 2), own, number, SEQ_DEV, EXPERTS, TOPK, SLOT, 2))(routes_keys, routes_turns).reshape((BATCH, TOPK))
    route_weight = jnp.clip(0.1 + 0.9 * jax.random.uniform(own_keys[21], (BATCH, TOPK), jnp.float32) ** block_levels(own_keys[21], (BATCH, TOPK), ((0, 16),), -0.2, 0.2), 0.1, 1.0)
    return dict(tokens_in=tokens_in, mix_gain=mix_gain, w_gate_z=w_gate_z, w_value=w_value, w_in_bc=w_in_bc, w_step=w_step, step_bias=step_bias, decay_log=decay_log, skip_gain=skip_gain, conv_x_weight=conv_x_weight, conv_bc_weight=conv_bc_weight, conv_x_state=conv_x_state, conv_bc_state=conv_bc_state, ssm_state=ssm_state, inner_gain=inner_gain, out_weight=out_weight, ffn_gain=ffn_gain, expert_gate=expert_gate, expert_up=expert_up, expert_down=expert_down, routes=routes, route_weight=route_weight)


def rms_norm(values, gain):
    floats = values.astype(jnp.float32)
    return floats * lax.rsqrt(lax.optimization_barrier(jnp.mean(floats * floats, axis=-1, keepdims=True)) + 1e-06) * gain

def conv_step(window_state, newest, taps):
    window = jnp.concatenate([window_state, newest[:, None, :]], axis=1)
    mixed = jax.nn.silu(lax.optimization_barrier(jnp.sum(window.astype(jnp.float32) * taps[None, :, :], axis=1)))
    return (mixed, window[:, 1:])

def reference(tokens_in, mix_gain, w_gate_z, w_value, w_in_bc, w_step, step_bias, decay_log, skip_gain, conv_x_weight, conv_bc_weight, conv_x_state, conv_bc_state, ssm_state, inner_gain, out_weight, ffn_gain, expert_gate, expert_up, expert_down, routes, route_weight):
    batch_rows = tokens_in.shape[0]
    normed = rms_norm(tokens_in, mix_gain).astype(jnp.bfloat16)
    z_pre = jnp.dot(normed, w_gate_z, preferred_element_type=jnp.float32).astype(jnp.bfloat16)
    x_pre = jnp.dot(normed, w_value, preferred_element_type=jnp.float32).astype(jnp.bfloat16)
    bc_pre = jnp.dot(normed, w_in_bc, preferred_element_type=jnp.float32).astype(jnp.bfloat16)
    step_pre = jnp.dot(normed, w_step, preferred_element_type=jnp.float32)
    x_conv, new_conv_x = conv_step(conv_x_state, x_pre, conv_x_weight)
    bc_conv, new_conv_bc = conv_step(conv_bc_state, bc_pre, conv_bc_weight)
    group_cols = GROUPS * NSTATE
    in_map = jnp.repeat(bc_conv[:, :group_cols].reshape(batch_rows, GROUPS, NSTATE), HEADS // GROUPS, axis=1)
    out_map = jnp.repeat(bc_conv[:, group_cols:].reshape(batch_rows, GROUPS, NSTATE), HEADS // GROUPS, axis=1)
    step = jax.nn.softplus(step_pre + step_bias[None, :])
    decay = jnp.exp(-step * jnp.exp(decay_log)[None, :])
    x_heads = x_conv.reshape(batch_rows, HEADS, HEAD_DIM)
    new_state = decay[:, :, None, None] * ssm_state + (step[:, :, None] * x_heads)[..., None] * in_map[:, :, None, :]
    head_out = jnp.einsum('bhn,bhpn->bhp', out_map, new_state, precision=lax.Precision.HIGHEST)
    head_out = head_out + skip_gain[None, :, None] * x_heads
    gated = head_out.reshape(batch_rows, HEADS * HEAD_DIM) * jax.nn.silu(z_pre.astype(jnp.float32))
    mixed = rms_norm(gated, inner_gain).astype(jnp.bfloat16)
    mix_out = jnp.dot(mixed, out_weight, preferred_element_type=jnp.float32).astype(jnp.bfloat16)
    resid = (tokens_in.astype(jnp.float32) + mix_out.astype(jnp.float32)).astype(jnp.bfloat16)
    ffn_in = rms_norm(resid, ffn_gain).astype(jnp.bfloat16)
    n_experts = expert_gate.shape[0]
    expert_ids = jnp.arange(n_experts, dtype=jnp.int32)
    dense_weight = lax.optimization_barrier(jnp.sum((routes[:, :, None] == expert_ids[None, None, :]).astype(jnp.float32) * route_weight[:, :, None], axis=1))

    def one_expert(total, index):
        gate_part = jnp.dot(ffn_in, expert_gate[index], preferred_element_type=jnp.float32)
        up_part = jnp.dot(ffn_in, expert_up[index], preferred_element_type=jnp.float32)
        act = (jax.nn.silu(gate_part) * up_part).astype(jnp.bfloat16)
        expert_row = jnp.dot(act, expert_down[index], preferred_element_type=jnp.float32).astype(jnp.bfloat16)
        column = lax.dynamic_slice_in_dim(dense_weight, index, 1, 1)
        return (total + column * expert_row.astype(jnp.float32), None)
    summed, _ = lax.scan(one_expert, jnp.zeros(tokens_in.shape, jnp.float32), expert_ids)
    out_tokens = (resid.astype(jnp.float32) + summed).astype(jnp.bfloat16)
    return (out_tokens, new_state, new_conv_x, new_conv_bc)
```

```python
import functools

import jax
import jax.numpy as jnp
from jax import lax
from jax.experimental import pallas as pl
from jax.experimental.pallas import tpu as pltpu
from jax.sharding import PartitionSpec as P

GROUPS = 4
NSTATE = 128
MESH = pl.DeviceIdType.MESH
F32 = jnp.float32
BF16 = jnp.bfloat16


def silu(v):
    return v * jax.nn.sigmoid(v)


def dot(a, b):
    return jnp.dot(a, b, preferred_element_type=F32)


def kernel(
    n,
    tok_ref,
    mixg_ref,
    sbias_ref,
    dlog_ref,
    skip_ref,
    cxw_ref,
    cbw_ref,
    cx_ref,
    cb_ref,
    innerg_ref,
    ffng_ref,
    routes_ref,
    rw_ref,
    wz_hbm,
    wv_hbm,
    wbc_hbm,
    wstep_hbm,
    state_hbm,
    wo_hbm,
    eg_hbm,
    eu_hbm,
    ed_hbm,
    out_ref,
    xpre_ref,
    bcpre_ref,
    nstate_hbm,
    wz,
    wv,
    wbc,
    wstep,
    state,
    wo,
    eg,
    eu,
    ed,
    buf1,
    send2,
    buf2,
    send3,
    buf3,
    send4,
    buf4,
    send5,
    buf5,
    toks,
    lhs,
    proj,
    small,
    step_b,
    decay_b,
    skip_x,
    convx,
    convbc,
    xconv,
    bcconv,
    zrow,
    xs,
    yrow,
    rows_f,
    lsem,
    ssem,
    rsem,
):
    me = lax.axis_index("ep")
    seq, width = tok_ref.shape
    heads = sbias_ref.shape[1]
    inner = cxw_ref.shape[1]
    hdim = inner // heads
    hgroup = heads // GROUPS
    zw, xw, bw = wz.shape[1], wv.shape[1], wbc.shape[1]
    ow = wo.shape[1]
    batch = n * seq

    barrier = pltpu.get_barrier_semaphore()

    def greet(k, c):
        pl.semaphore_signal(
            barrier, inc=1, device_id={"ep": lax.rem(me + k, n)}, device_id_type=MESH
        )
        return c

    lax.fori_loop(1, n, greet, 0)

    loads = [
        pltpu.make_async_copy(src, dst, lsem.at[i])
        for i, (src, dst) in enumerate(
            (
                (wstep_hbm, wstep),
                (wz_hbm, wz),
                (wv_hbm, wv),
                (wbc_hbm, wbc),
                (state_hbm, state),
                (wo_hbm, wo),
                (eg_hbm.at[0], eg),
                (eu_hbm.at[0], eu),
                (ed_hbm.at[0], ed),
            )
        )
    ]
    for load in loads:
        load.start()

    def remote(phase, src, dst, peer, slot):
        return pltpu.make_async_remote_copy(
            src_ref=src,
            dst_ref=dst,
            send_sem=ssem.at[phase, slot],
            recv_sem=rsem.at[phase, slot],
            device_id={"ep": peer},
            device_id_type=MESH,
        )

    def send_all(phase, src_of, buf):
        def body(k, c):
            peer = lax.rem(me + k, n)
            pltpu.make_async_remote_copy(
                src_ref=src_of(peer),
                dst_ref=buf.at[me],
                send_sem=ssem.at[phase, peer],
                recv_sem=rsem.at[phase, me],
                device_id={"ep": peer},
                device_id_type=MESH,
            ).start()
            return c

        lax.fori_loop(1, n, body, 0)

    def recv_all(phase, src_of, buf):
        def body(k, c):
            peer = lax.rem(me + n - k, n)
            remote(phase, src_of(peer), buf.at[peer], peer, peer).wait_recv()
            return c

        lax.fori_loop(1, n, body, 0)

    def drain(phase, src_of, buf):
        def body(k, c):
            peer = lax.rem(me + k, n)
            remote(phase, src_of(peer), buf.at[peer], peer, peer).wait_send()
            return c

        lax.fori_loop(1, n, body, 0)

    pl.semaphore_wait(barrier, n - 1)

    whole1 = lambda peer: tok_ref
    send_all(0, whole1, buf1)
    buf1[me] = tok_ref[...]

    own = tok_ref[...].astype(F32)
    own_normed = (
        own * lax.rsqrt(jnp.mean(own * own, axis=-1, keepdims=True) + 1e-06) * mixg_ref[...]
    ).astype(BF16)
    loads[0].wait()
    pre = dot(own_normed, wstep[...]) + sbias_ref[...]
    step = jnp.maximum(pre, 0.0) + jnp.log1p(jnp.exp(-jnp.abs(pre)))
    decay = jnp.exp(-step * jnp.exp(dlog_ref[...]))
    small[...] = jnp.zeros_like(small)
    small[0:seq, 0:heads] = step
    small[seq : 2 * seq, 0:heads] = decay
    small[2 * seq : 2 * seq + 1, 0:heads] = skip_ref[...]
    turned = jnp.transpose(small[...])
    for b in range(seq):
        step_b[b] = jnp.broadcast_to(turned[0:heads, b : b + 1], (heads, NSTATE))
        decay_b[b] = jnp.broadcast_to(
            turned[0:heads, seq + b : seq + b + 1], (heads, NSTATE)
        )
    skips = jnp.broadcast_to(turned[0:heads, 2 * seq : 2 * seq + 1], (heads, NSTATE))
    per = 128 // hdim
    lane = lax.broadcasted_iota(jnp.int32, (1, 128), 1)
    for r in range(inner // 128):
        row = skips[per * r : per * r + 1]
        for j in range(1, per):
            row = jnp.where(lane < j * hdim, row, skips[per * r + j : per * r + j + 1])
        skip_x[:, 128 * r : 128 * r + 128] = row
    taps = cx_ref.shape[1]
    for b in range(seq):
        convx[b : b + 1, :] = jnp.sum(
            cx_ref[b].astype(F32) * cxw_ref[0:taps, :], axis=0, keepdims=True
        )
        convbc[b : b + 1, :] = jnp.sum(
            cb_ref[b].astype(F32) * cbw_ref[0:taps, :], axis=0, keepdims=True
        )

    recv_all(0, whole1, buf1)
    for s in range(n):
        toks[seq * s : seq * s + seq, :] = buf1[s].astype(F32)
    t = toks[...]
    scale = lax.rsqrt(jnp.mean(t * t, axis=-1, keepdims=True) + 1e-06)
    lhs[...] = (toks[...] * scale * mixg_ref[...]).astype(BF16)
    loads[1].wait()
    proj[:, 0:zw] = dot(lhs[...], wz[...])
    loads[2].wait()
    proj[:, zw : zw + xw] = dot(lhs[...], wv[...])
    loads[3].wait()
    proj[:, zw + xw : zw + xw + bw] = dot(lhs[...], wbc[...])
    for s in range(n):
        send2[s] = proj[seq * s : seq * s + seq, :].astype(BF16)
    slot2 = lambda peer: send2.at[peer]
    send_all(1, slot2, buf2)
    buf2[me] = send2[me]
    recv_all(1, slot2, buf2)
    for s in range(n):
        zrow[:, zw * s : zw * s + zw] = buf2[s, :, 0:zw].astype(F32)
        xpre_ref[:, xw * s : xw * s + xw] = buf2[s, :, zw : zw + xw]
        bcpre_ref[:, bw * s : bw * s + bw] = buf2[s, :, zw + xw : zw + xw + bw]

    xconv[...] = silu(convx[...] + xpre_ref[...].astype(F32) * cxw_ref[taps : taps + 1, :])
    bcconv[...] = silu(convbc[...] + bcpre_ref[...].astype(F32) * cbw_ref[taps : taps + 1, :])
    chunks = hgroup // per
    for g in range(GROUPS):
        for r in range(chunks):
            at = 128 * (chunks * g + r)
            xs[g, seq * r : seq * r + seq, :] = xconv[:, at : at + 128]

    loads[4].wait()

    def group(g, c):
        cols = jnp.transpose(xs[g])
        hs = pl.ds(pl.multiple_of(g * hgroup, hgroup), hgroup)
        for b in range(seq):
            at = pl.multiple_of(g * NSTATE, NSTATE)
            in_map = bcconv[b : b + 1, pl.ds(at, NSTATE)]
            out_at = pl.multiple_of((GROUPS + g) * NSTATE, NSTATE)
            out_map = bcconv[b : b + 1, pl.ds(out_at, NSTATE)]
            ins = step_b[b, hs, :] * in_map
            decs = decay_b[b, hs, :]
            for h in range(hgroup):
                r, j = h // per, h % per
                col = cols[hdim * j : hdim * j + hdim, seq * r + b : seq * r + b + 1]
                state[b, g * hgroup + h] = (
                    decs[h : h + 1] * state[b, g * hgroup + h] + col * ins[h : h + 1]
                )
            new = state[b, hs].reshape(hgroup * hdim, NSTATE).astype(BF16)
            left = jnp.broadcast_to(out_map, (8, NSTATE)).astype(BF16)
            y = lax.dot_general(
                left, new, (((1,), (1,)), ((), ())), preferred_element_type=F32
            )
            yrow[b : b + 1, pl.ds(pl.multiple_of(g * hgroup * hdim, 128), hgroup * hdim)] = y[0:1]
        return c

    lax.fori_loop(0, GROUPS, group, 0)
    store = pltpu.make_async_copy(state, nstate_hbm, lsem.at[len(loads)])
    store.start()

    gated = (yrow[...] + skip_x[...] * xconv[...]) * silu(zrow[...])
    mixed = (
        gated
        * lax.rsqrt(jnp.mean(gated * gated, axis=-1, keepdims=True) + 1e-06)
        * innerg_ref[...]
    ).astype(BF16)
    send3[...] = mixed
    whole3 = lambda peer: send3
    send_all(2, whole3, buf3)
    buf3[me] = mixed
    recv_all(2, whole3, buf3)
    for s in range(n):
        rows_f[seq * s : seq * s + seq, :] = buf3[s].astype(F32)
    lhs[...] = rows_f[...].astype(BF16)
    loads[5].wait()
    cols_out = dot(lhs[...], wo[...]).astype(BF16)
    send4[...] = cols_out
    whole4 = lambda peer: send4
    send_all(3, whole4, buf4)
    buf4[me] = cols_out
    recv_all(3, whole4, buf4)

    for s in range(n):
        at = slice(ow * s, ow * s + ow)
        rows_f[:, at] = (toks[:, at] + buf4[s].astype(F32)).astype(BF16).astype(F32)
    t = rows_f[...]
    scale = lax.rsqrt(jnp.mean(t * t, axis=-1, keepdims=True) + 1e-06)
    lhs[...] = (rows_f[...] * scale * ffng_ref[...]).astype(BF16)
    for b in range(seq):
        yrow[b : b + 1, :] = rows_f[pl.ds(me * seq + b, 1), :]
    loads[6].wait()
    gate_part = dot(lhs[...], eg[...])
    loads[7].wait()
    up_part = dot(lhs[...], eu[...])
    act = (silu(gate_part) * up_part).astype(BF16)
    loads[8].wait()
    piece = 512
    for i in range(width // piece):
        at = slice(i * piece, i * piece + piece)
        part = dot(act, ed[:, at])
        for s in range(n):
            send5[s, :, at] = part[seq * s : seq * s + seq].astype(BF16)
    slot5 = lambda peer: send5.at[peer]
    send_all(4, slot5, buf5)
    buf5[me] = send5[me]
    drain(0, whole1, buf1)
    drain(1, slot2, buf2)
    drain(2, whole3, buf3)
    drain(3, whole4, buf4)
    recv_all(4, slot5, buf5)
    total = yrow[...]
    for e in range(n):
        w = jnp.sum(jnp.where(routes_ref[...] == e, rw_ref[...], 0.0), axis=1, keepdims=True)
        total = total + w * buf5[e].astype(F32)
    out_ref[...] = total.astype(BF16)
    drain(4, slot5, buf5)
    store.wait()


def body(
    tokens_in,
    mix_gain,
    w_gate_z,
    w_value,
    w_in_bc,
    w_step,
    step_bias,
    decay_log,
    skip_gain,
    conv_x_weight,
    conv_bc_weight,
    conv_x_state,
    conv_bc_state,
    ssm_state,
    inner_gain,
    out_weight,
    ffn_gain,
    expert_gate,
    expert_up,
    expert_down,
    routes,
    route_weight,
):
    n = lax.axis_size("ep")
    seq, width = tokens_in.shape
    heads = step_bias.shape[0]
    inner = conv_x_weight.shape[1]
    bcw = conv_bc_weight.shape[1]
    zw, xw, bw = w_gate_z.shape[1], w_value.shape[1], w_in_bc.shape[1]
    pw = zw + xw + bw
    ow = out_weight.shape[1]
    batch = n * seq
    vmem = pl.BlockSpec(memory_space=pltpu.VMEM)
    hbm = pl.BlockSpec(memory_space=pl.ANY)
    chunk_rows = heads // GROUPS * (inner // heads) // 128 * seq
    scratch = [
        pltpu.VMEM(w_gate_z.shape, BF16),
        pltpu.VMEM(w_value.shape, BF16),
        pltpu.VMEM(w_in_bc.shape, BF16),
        pltpu.VMEM(w_step.shape, BF16),
        pltpu.VMEM(ssm_state.shape, F32),
        pltpu.VMEM(out_weight.shape, BF16),
        pltpu.VMEM(expert_gate.shape[1:], BF16),
        pltpu.VMEM(expert_up.shape[1:], BF16),
        pltpu.VMEM(expert_down.shape[1:], BF16),
        pltpu.VMEM((n, seq, width), BF16),
        pltpu.VMEM((n, seq, pw), BF16),
        pltpu.VMEM((n, seq, pw), BF16),
        pltpu.VMEM((seq, inner), BF16),
        pltpu.VMEM((n, seq, inner), BF16),
        pltpu.VMEM((batch, ow), BF16),
        pltpu.VMEM((n, batch, ow), BF16),
        pltpu.VMEM((n, seq, width), BF16),
        pltpu.VMEM((n, seq, width), BF16),
        pltpu.VMEM((batch, width), F32),
        pltpu.VMEM((batch, width), BF16),
        pltpu.VMEM((batch, pw), F32),
        pltpu.VMEM((128, 128), F32),
        pltpu.VMEM((seq, heads, NSTATE), F32),
        pltpu.VMEM((seq, heads, NSTATE), F32),
        pltpu.VMEM((1, inner), F32),
        pltpu.VMEM((seq, inner), F32),
        pltpu.VMEM((seq, bcw), F32),
        pltpu.VMEM((seq, inner), F32),
        pltpu.VMEM((seq, bcw), F32),
        pltpu.VMEM((seq, inner), F32),
        pltpu.VMEM((GROUPS, chunk_rows, 128), F32),
        pltpu.VMEM((seq, inner), F32),
        pltpu.VMEM((batch, width), F32),
        pltpu.SemaphoreType.DMA((10,)),
        pltpu.SemaphoreType.DMA((5, n)),
        pltpu.SemaphoreType.DMA((5, n)),
    ]
    out_tokens, x_pre, bc_pre, new_state = pl.pallas_call(
        functools.partial(kernel, n),
        out_shape=(
            jax.ShapeDtypeStruct((seq, width), BF16),
            jax.ShapeDtypeStruct((seq, inner), BF16),
            jax.ShapeDtypeStruct((seq, bcw), BF16),
            jax.ShapeDtypeStruct(ssm_state.shape, F32),
        ),
        in_specs=[vmem] * 13 + [hbm] * 9,
        out_specs=(vmem, vmem, vmem, hbm),
        scratch_shapes=scratch,
        compiler_params=pltpu.CompilerParams(
            collective_id=0, has_side_effects=True, vmem_limit_bytes=60 * 1024 * 1024
        ),
    )(
        tokens_in,
        mix_gain[None, :],
        step_bias[None, :],
        decay_log[None, :],
        skip_gain[None, :],
        conv_x_weight,
        conv_bc_weight,
        conv_x_state,
        conv_bc_state,
        inner_gain[None, :],
        ffn_gain[None, :],
        routes,
        route_weight,
        w_gate_z,
        w_value,
        w_in_bc,
        w_step,
        ssm_state,
        out_weight,
        expert_gate,
        expert_up,
        expert_down,
    )
    new_conv_x = jnp.concatenate([conv_x_state[:, 1:], x_pre[:, None, :]], axis=1)
    new_conv_bc = jnp.concatenate([conv_bc_state[:, 1:], bc_pre[:, None, :]], axis=1)
    return (out_tokens, new_state, new_conv_x, new_conv_bc)


def solution(mesh):
    rows = P(("grp", "ep"), None)
    placed = (
        rows,
        P(),
        P(None, "ep"),
        P(None, "ep"),
        P(None, "ep"),
        P(),
        P(),
        P(),
        P(),
        P(),
        P(),
        P(("grp", "ep"), None, None),
        P(("grp", "ep"), None, None),
        P(("grp", "ep"), None, None, None),
        P(),
        P(None, "ep"),
        P(),
        P("ep", None, None),
        P("ep", None, None),
        P("ep", None, None),
        rows,
        rows,
    )
    return jax.shard_map(
        body,
        mesh=mesh,
        in_specs=placed,
        out_specs=(
            rows,
            P(("grp", "ep"), None, None, None),
            P(("grp", "ep"), None, None),
            P(("grp", "ep"), None, None),
        ),
        check_vma=False,
    )
```

```python
import functools

import jax
import jax.numpy as jnp
from jax import lax
from jax.experimental import pallas as pl
from jax.experimental.pallas import tpu as pltpu
from jax.sharding import PartitionSpec as P

GROUPS = 4
NSTATE = 128
MESH = pl.DeviceIdType.MESH
F32 = jnp.float32
BF16 = jnp.bfloat16


def silu(v):
    return v * jax.nn.sigmoid(v)


def dot(a, b):
    return jnp.dot(a, b, preferred_element_type=F32)


def dot_t(a, b):
    return lax.dot_general(a, b, (((1,), (1,)), ((), ())), preferred_element_type=F32)


def kernel(
    n,
    tok_ref,
    mixg_ref,
    sbias_ref,
    dlog_ref,
    skip_ref,
    cxw_ref,
    cbw_ref,
    cx_ref,
    cb_ref,
    innerg_ref,
    ffng_ref,
    routes_ref,
    rw_ref,
    wz_hbm,
    wv_hbm,
    wbc_hbm,
    wstep_hbm,
    state_hbm,
    wo_hbm,
    eg_hbm,
    eu_hbm,
    ed_hbm,
    out_ref,
    ncx_ref,
    ncb_ref,
    nstate_ref,
    wz,
    wv,
    wbc,
    wstep,
    state,
    wo,
    eg,
    eu,
    ed,
    buf1,
    send2,
    buf2,
    send3,
    buf3,
    send4,
    buf4,
    send5,
    buf5,
    toks,
    lhs,
    proj,
    small,
    step_b,
    decay_b,
    skip_x,
    step_x,
    decay_x,
    state16,
    convx,
    convbc,
    xconv,
    bcconv,
    zrow,
    xs,
    yrow,
    rows_f,
    lsem,
    ssem,
    rsem,
):
    me = lax.axis_index("ep")
    seq, width = tok_ref.shape
    heads = sbias_ref.shape[1]
    inner = cxw_ref.shape[1]
    hdim = inner // heads
    hgroup = heads // GROUPS
    zw, xw, bw = wz.shape[1], wv.shape[1], wbc.shape[0]
    ow = wo.shape[1]
    batch = n * seq

    barrier = pltpu.get_barrier_semaphore()

    def greet(k, c):
        pl.semaphore_signal(
            barrier, inc=1, device_id={"ep": lax.rem(me + k, n)}, device_id_type=MESH
        )
        return c

    lax.fori_loop(1, n, greet, 0)

    loads = [
        pltpu.make_async_copy(src, dst, lsem.at[i])
        for i, (src, dst) in enumerate(
            (
                (wstep_hbm, wstep),
                (wz_hbm, wz),
                (wv_hbm, wv),
                (wbc_hbm, wbc),
                (state_hbm, state),
                (wo_hbm, wo),
                (eg_hbm.at[0], eg),
                (eu_hbm.at[0], eu),
                (ed_hbm.at[0], ed),
            )
        )
    ]
    for load in loads:
        load.start()

    def remote(phase, src, dst, peer, slot):
        return pltpu.make_async_remote_copy(
            src_ref=src,
            dst_ref=dst,
            send_sem=ssem.at[phase, slot],
            recv_sem=rsem.at[phase, slot],
            device_id={"ep": peer},
            device_id_type=MESH,
        )

    def send_all(phase, src_of, buf):
        def body(k, c):
            peer = lax.rem(me + k, n)
            pltpu.make_async_remote_copy(
                src_ref=src_of(peer),
                dst_ref=buf.at[me],
                send_sem=ssem.at[phase, peer],
                recv_sem=rsem.at[phase, me],
                device_id={"ep": peer},
                device_id_type=MESH,
            ).start()
            return c

        lax.fori_loop(1, n, body, 0)

    def recv_all(phase, src_of, buf):
        def body(k, c):
            peer = lax.rem(me + n - k, n)
            remote(phase, src_of(peer), buf.at[peer], peer, peer).wait_recv()
            return c

        lax.fori_loop(1, n, body, 0)

    def drain(phase, src_of, buf):
        def body(k, c):
            peer = lax.rem(me + k, n)
            remote(phase, src_of(peer), buf.at[peer], peer, peer).wait_send()
            return c

        lax.fori_loop(1, n, body, 0)

    pl.semaphore_wait(barrier, n - 1)

    whole1 = lambda peer: tok_ref
    send_all(0, whole1, buf1)
    buf1[me] = tok_ref[...]

    own = tok_ref[...].astype(F32)
    own_normed = (
        own * lax.rsqrt(jnp.mean(own * own, axis=-1, keepdims=True) + 1e-06) * mixg_ref[...]
    ).astype(BF16)
    loads[0].wait()
    pre = dot_t(own_normed, wstep[...]) + sbias_ref[...]
    step = jnp.maximum(pre, 0.0) + jnp.log1p(jnp.exp(-jnp.abs(pre)))
    decay = jnp.exp(-step * jnp.exp(dlog_ref[...]))
    small[...] = jnp.zeros_like(small)
    small[0:seq, 0:heads] = step
    small[seq : 2 * seq, 0:heads] = decay
    small[2 * seq : 2 * seq + 1, 0:heads] = skip_ref[...]
    turned = jnp.transpose(small[...])
    for b in range(seq):
        step_b[b] = jnp.broadcast_to(turned[0:heads, b : b + 1], (heads, NSTATE))
        decay_b[b] = jnp.broadcast_to(
            turned[0:heads, seq + b : seq + b + 1], (heads, NSTATE)
        )
    rows_b = jnp.broadcast_to(turned[0:heads, 2 * seq : 2 * seq + 1], (heads, NSTATE))
    per = 128 // hdim
    lane = lax.broadcasted_iota(jnp.int32, (1, 128), 1)

    def spread(value, dst, at):
        for r in range(inner // 128):
            row = value[per * r : per * r + 1]
            for j in range(1, per):
                row = jnp.where(lane < j * hdim, row, value[per * r + j : per * r + j + 1])
            dst[at : at + 1, 128 * r : 128 * r + 128] = row

    spread(rows_b, skip_x, 0)
    for b in range(seq):
        spread(step_b[b], step_x, b)
        spread(decay_b[b], decay_x, b)
    taps = cx_ref.shape[0]
    for state_ref, weight_ref, sum_ref, new_ref in (
        (cx_ref, cxw_ref, convx, ncx_ref),
        (cb_ref, cbw_ref, convbc, ncb_ref),
    ):
        total = state_ref[0].astype(F32) * weight_ref[0:1, :]
        for i in range(1, taps):
            new_ref[i - 1] = state_ref[i]
            total = total + state_ref[i].astype(F32) * weight_ref[i : i + 1, :]
        sum_ref[...] = total

    recv_all(0, whole1, buf1)
    for s in range(n):
        toks[seq * s : seq * s + seq, :] = buf1[s].astype(F32)
    t = toks[...]
    scale = lax.rsqrt(jnp.mean(t * t, axis=-1, keepdims=True) + 1e-06)
    lhs[...] = (toks[...] * scale * mixg_ref[...]).astype(BF16)
    loads[1].wait()
    proj[:, 0:zw] = dot(lhs[...], wz[...])
    loads[2].wait()
    proj[:, zw : zw + xw] = dot(lhs[...], wv[...])
    loads[3].wait()
    proj[:, zw + xw : zw + xw + bw] = dot_t(lhs[...], wbc[...])
    for s in range(n):
        send2[s] = proj[seq * s : seq * s + seq, :].astype(BF16)
    slot2 = lambda peer: send2.at[peer]
    send_all(1, slot2, buf2)
    buf2[me] = send2[me]
    loads[4].wait()

    def narrow(g, c):
        hs = pl.ds(pl.multiple_of(g * hgroup, hgroup), hgroup)
        for b in range(seq):
            state16[b, g] = state[b, hs].reshape(hgroup * hdim, NSTATE).astype(BF16)
        return c

    lax.fori_loop(0, GROUPS, narrow, 0)
    recv_all(1, slot2, buf2)
    for s in range(n):
        zrow[:, zw * s : zw * s + zw] = buf2[s, :, 0:zw].astype(F32)
        ncx_ref[taps - 1, :, xw * s : xw * s + xw] = buf2[s, :, zw : zw + xw]
        ncb_ref[taps - 1, :, bw * s : bw * s + bw] = buf2[s, :, zw + xw : zw + xw + bw]

    xconv[...] = silu(convx[...] + ncx_ref[taps - 1].astype(F32) * cxw_ref[taps : taps + 1, :])
    bcconv[...] = silu(convbc[...] + ncb_ref[taps - 1].astype(F32) * cbw_ref[taps : taps + 1, :])
    gw = hgroup * hdim
    for g in range(GROUPS):
        at = slice(g * gw, g * gw + gw)
        for b in range(seq):
            in_map = bcconv[b : b + 1, g * NSTATE : (g + 1) * NSTATE]
            out_map = bcconv[b : b + 1, (GROUPS + g) * NSTATE : (GROUPS + g + 1) * NSTATE]
            meet = jnp.sum(in_map * out_map, axis=1, keepdims=True)
            left = jnp.broadcast_to(out_map, (8, NSTATE)).astype(BF16)
            y = dot_t(left, state16[b, g])
            yrow[b : b + 1, at] = (
                decay_x[b : b + 1, at] * y[0:1]
                + (meet * step_x[b : b + 1, at] + skip_x[:, at]) * xconv[b : b + 1, at]
            )
    gated = yrow[...] * silu(zrow[...])
    mixed = (
        gated
        * lax.rsqrt(jnp.mean(gated * gated, axis=-1, keepdims=True) + 1e-06)
        * innerg_ref[...]
    ).astype(BF16)
    send3[...] = mixed
    whole3 = lambda peer: send3
    send_all(2, whole3, buf3)
    buf3[me] = mixed
    chunks = hgroup // per
    for g in range(GROUPS):
        for r in range(chunks):
            at = 128 * (chunks * g + r)
            xs[g, seq * r : seq * r + seq, :] = xconv[:, at : at + 128]

    def group(g, c):
        cols = jnp.transpose(xs[g])
        hs = pl.ds(pl.multiple_of(g * hgroup, hgroup), hgroup)
        for b in range(seq):
            at = pl.multiple_of(g * NSTATE, NSTATE)
            ins = step_b[b, hs, :] * bcconv[b : b + 1, pl.ds(at, NSTATE)]
            decs = decay_b[b, hs, :]
            for h in range(hgroup):
                r, j = h // per, h % per
                col = cols[hdim * j : hdim * j + hdim, seq * r + b : seq * r + b + 1]
                nstate_ref[b, g * hgroup + h] = (
                    decs[h : h + 1] * state[b, g * hgroup + h] + col * ins[h : h + 1]
                )
        return c

    lax.fori_loop(0, GROUPS, group, 0)
    recv_all(2, whole3, buf3)
    for s in range(n):
        rows_f[seq * s : seq * s + seq, :] = buf3[s].astype(F32)
    lhs[...] = rows_f[...].astype(BF16)
    loads[5].wait()
    cols_out = dot(lhs[...], wo[...]).astype(BF16)
    send4[...] = cols_out
    whole4 = lambda peer: send4
    send_all(3, whole4, buf4)
    buf4[me] = cols_out
    recv_all(3, whole4, buf4)

    for s in range(n):
        at = slice(ow * s, ow * s + ow)
        rows_f[:, at] = (toks[:, at] + buf4[s].astype(F32)).astype(BF16).astype(F32)
    t = rows_f[...]
    scale = lax.rsqrt(jnp.mean(t * t, axis=-1, keepdims=True) + 1e-06)
    lhs[...] = (rows_f[...] * scale * ffng_ref[...]).astype(BF16)
    for b in range(seq):
        yrow[b : b + 1, :] = rows_f[pl.ds(me * seq + b, 1), :]
    loads[6].wait()
    gate_part = dot(lhs[...], eg[...])
    loads[7].wait()
    up_part = dot(lhs[...], eu[...])
    act = (silu(gate_part) * up_part).astype(BF16)
    loads[8].wait()
    piece = 512
    for i in range(width // piece):
        at = slice(i * piece, i * piece + piece)
        part = dot(act, ed[:, at])
        for s in range(n):
            send5[s, :, at] = part[seq * s : seq * s + seq].astype(BF16)
    slot5 = lambda peer: send5.at[peer]
    send_all(4, slot5, buf5)
    buf5[me] = send5[me]
    drain(0, whole1, buf1)
    drain(1, slot2, buf2)
    drain(2, whole3, buf3)
    drain(3, whole4, buf4)
    recv_all(4, slot5, buf5)
    total = yrow[...]
    for e in range(n):
        w = jnp.sum(jnp.where(routes_ref[...] == e, rw_ref[...], 0.0), axis=1, keepdims=True)
        total = total + w * buf5[e].astype(F32)
    out_ref[...] = total.astype(BF16)
    drain(4, slot5, buf5)


def hand_over(*refs):
    sem = refs[8]
    moves = [pltpu.make_async_copy(refs[i], refs[4 + i], sem.at[i]) for i in range(4)]
    for move in reversed(moves):
        move.start()
    for move in moves:
        move.wait()


def body(
    tokens_in,
    mix_gain,
    w_gate_z,
    w_value,
    w_in_bc,
    w_step,
    step_bias,
    decay_log,
    skip_gain,
    conv_x_weight,
    conv_bc_weight,
    conv_x_state,
    conv_bc_state,
    ssm_state,
    inner_gain,
    out_weight,
    ffn_gain,
    expert_gate,
    expert_up,
    expert_down,
    routes,
    route_weight,
):
    n = lax.axis_size("ep")
    seq, width = tokens_in.shape
    heads = step_bias.shape[0]
    inner = conv_x_weight.shape[1]
    bcw = conv_bc_weight.shape[1]
    taps = conv_x_state.shape[1]
    zw, xw, bw = w_gate_z.shape[1], w_value.shape[1], w_in_bc.shape[1]
    pw = zw + xw + bw
    ow = out_weight.shape[1]
    batch = n * seq
    vmem = pl.BlockSpec(memory_space=pltpu.VMEM)
    hbm = pl.BlockSpec(memory_space=pltpu.HBM)
    chunk_rows = heads // GROUPS * (inner // heads) // 128 * seq
    scratch = [
        pltpu.VMEM(w_gate_z.shape, BF16),
        pltpu.VMEM(w_value.shape, BF16),
        pltpu.VMEM(w_in_bc.shape[::-1], BF16),
        pltpu.VMEM(w_step.shape[::-1], BF16),
        pltpu.VMEM(ssm_state.shape, F32),
        pltpu.VMEM(out_weight.shape, BF16),
        pltpu.VMEM(expert_gate.shape[1:], BF16),
        pltpu.VMEM(expert_up.shape[1:], BF16),
        pltpu.VMEM(expert_down.shape[1:], BF16),
        pltpu.VMEM((n, seq, width), BF16),
        pltpu.VMEM((n, seq, pw), BF16),
        pltpu.VMEM((n, seq, pw), BF16),
        pltpu.VMEM((seq, inner), BF16),
        pltpu.VMEM((n, seq, inner), BF16),
        pltpu.VMEM((batch, ow), BF16),
        pltpu.VMEM((n, batch, ow), BF16),
        pltpu.VMEM((n, seq, width), BF16),
        pltpu.VMEM((n, seq, width), BF16),
        pltpu.VMEM((batch, width), F32),
        pltpu.VMEM((batch, width), BF16),
        pltpu.VMEM((batch, pw), F32),
        pltpu.VMEM((128, 128), F32),
        pltpu.VMEM((seq, heads, NSTATE), F32),
        pltpu.VMEM((seq, heads, NSTATE), F32),
        pltpu.VMEM((1, inner), F32),
        pltpu.VMEM((seq, inner), F32),
        pltpu.VMEM((seq, inner), F32),
        pltpu.VMEM((seq, GROUPS, inner // GROUPS, NSTATE), BF16),
        pltpu.VMEM((seq, inner), F32),
        pltpu.VMEM((seq, bcw), F32),
        pltpu.VMEM((seq, inner), F32),
        pltpu.VMEM((seq, bcw), F32),
        pltpu.VMEM((seq, inner), F32),
        pltpu.VMEM((GROUPS, chunk_rows, 128), F32),
        pltpu.VMEM((seq, inner), F32),
        pltpu.VMEM((batch, width), F32),
        pltpu.SemaphoreType.DMA((9,)),
        pltpu.SemaphoreType.DMA((5, n)),
        pltpu.SemaphoreType.DMA((5, n)),
    ]
    results = pl.pallas_call(
        functools.partial(kernel, n),
        out_shape=(
            jax.ShapeDtypeStruct((seq, width), BF16),
            jax.ShapeDtypeStruct((taps, seq, inner), BF16),
            jax.ShapeDtypeStruct((taps, seq, bcw), BF16),
            pltpu.VMEM(ssm_state.shape, F32),
        ),
        in_specs=[vmem] * 13 + [hbm] * 9,
        out_specs=(vmem, vmem, vmem, vmem),
        scratch_shapes=scratch,
        compiler_params=pltpu.CompilerParams(
            collective_id=0, has_side_effects=True, vmem_limit_bytes=44 * 1024 * 1024
        ),
    )(
        tokens_in,
        mix_gain[None, :],
        step_bias[None, :],
        decay_log[None, :],
        skip_gain[None, :],
        conv_x_weight,
        conv_bc_weight,
        jnp.transpose(conv_x_state, (1, 0, 2)),
        jnp.transpose(conv_bc_state, (1, 0, 2)),
        inner_gain[None, :],
        ffn_gain[None, :],
        routes,
        route_weight,
        *(
            pltpu.with_memory_space_constraint(v, pltpu.HBM)
            for v in (
                w_gate_z,
                w_value,
                w_in_bc.T,
                w_step.T,
                ssm_state,
                out_weight,
                expert_gate,
                expert_up,
                expert_down,
            )
        ),
    )
    out_tokens, new_x, new_bc, new_state = pl.pallas_call(
        hand_over,
        out_shape=tuple(jax.ShapeDtypeStruct(r.shape, r.dtype) for r in results),
        in_specs=[vmem] * 4,
        out_specs=(hbm,) * 4,
        scratch_shapes=[pltpu.SemaphoreType.DMA((4,))],
        compiler_params=pltpu.CompilerParams(vmem_limit_bytes=8 * 1024 * 1024),
    )(*results)
    return (
        out_tokens,
        new_state,
        jnp.transpose(new_x, (1, 0, 2)),
        jnp.transpose(new_bc, (1, 0, 2)),
    )


def solution(mesh):
    rows = P(("grp", "ep"), None)
    placed = (
        rows,
        P(),
        P(None, "ep"),
        P(None, "ep"),
        P(None, "ep"),
        P(),
        P(),
        P(),
        P(),
        P(),
        P(),
        P(("grp", "ep"), None, None),
        P(("grp", "ep"), None, None),
        P(("grp", "ep"), None, None, None),
        P(),
        P(None, "ep"),
        P(),
        P("ep", None, None),
        P("ep", None, None),
        P("ep", None, None),
        rows,
        rows,
    )
    return jax.shard_map(
        body,
        mesh=mesh,
        in_specs=placed,
        out_specs=(
            rows,
            P(("grp", "ep"), None, None, None),
            P(("grp", "ep"), None, None),
            P(("grp", "ep"), None, None),
        ),
        check_vma=False,
    )
```

```python
import functools

import jax
import jax.numpy as jnp
from jax import lax
from jax.experimental import pallas as pl
from jax.experimental.pallas import tpu as pltpu
from jax.sharding import PartitionSpec as P

GROUPS = 4
NSTATE = 128
MESH = pl.DeviceIdType.MESH
F32 = jnp.float32
BF16 = jnp.bfloat16


def silu(v):
    return v * jax.nn.sigmoid(v)


def dot(a, b):
    return jnp.dot(a, b, preferred_element_type=F32)


def dot_t(a, b):
    return lax.dot_general(a, b, (((1,), (1,)), ((), ())), preferred_element_type=F32)


SMALLS = 13
REFS = SMALLS + 13


def kernel(
    n,
    fills,
    tok_ref,
    mixg_ref,
    sbias_ref,
    dlog_ref,
    skip_ref,
    cxw_ref,
    cbw_ref,
    cx_ref,
    cb_ref,
    innerg_ref,
    ffng_ref,
    routes_ref,
    rw_ref,
    wz_hbm,
    wv_hbm,
    wbc_hbm,
    wstep_hbm,
    state_hbm,
    wo_hbm,
    eg_hbm,
    eu_hbm,
    ed_hbm,
    out_ref,
    ncx_ref,
    ncb_ref,
    nstate_ref,
    wz,
    wv,
    wbc,
    wstep,
    state,
    wo,
    eg,
    eu,
    ed,
    buf1,
    send2,
    buf2,
    send3,
    buf3,
    send4,
    buf4,
    send5,
    buf5,
    toks,
    lhs,
    proj,
    small,
    step_b,
    decay_b,
    skip_x,
    step_x,
    decay_x,
    state16,
    convx,
    convbc,
    xconv,
    bcconv,
    zrow,
    xs,
    yrow,
    rows_f,
    lsem,
    ssem,
    rsem,
):
    me = lax.axis_index("ep")
    seq, width = tok_ref.shape
    heads = sbias_ref.shape[1]
    inner = cxw_ref.shape[1]
    hdim = inner // heads
    hgroup = heads // GROUPS
    zw, xw, bw = wz.shape[1], wv.shape[1], wbc.shape[0]
    ow = wo.shape[1]
    batch = n * seq

    barrier = pltpu.get_barrier_semaphore()

    def greet(k, c):
        pl.semaphore_signal(
            barrier, inc=1, device_id={"ep": lax.rem(me + k, n)}, device_id_type=MESH
        )
        return c

    lax.fori_loop(1, n, greet, 0)

    loads = [
        pltpu.make_async_copy(src, dst, lsem.at[i])
        for i, (src, dst) in enumerate(
            (
                (wstep_hbm, wstep),
                (wz_hbm, wz),
                (wv_hbm, wv),
                (wbc_hbm, wbc),
                (state_hbm, state),
                (wo_hbm, wo),
                (eg_hbm.at[0], eg),
                (eu_hbm.at[0], eu),
                (ed_hbm.at[0], ed),
            )
        )
    ]
    for load in fills + loads:
        load.start()

    def remote(phase, src, dst, peer, slot):
        return pltpu.make_async_remote_copy(
            src_ref=src,
            dst_ref=dst,
            send_sem=ssem.at[phase, slot],
            recv_sem=rsem.at[phase, slot],
            device_id={"ep": peer},
            device_id_type=MESH,
        )

    def send_all(phase, src_of, buf):
        def body(k, c):
            peer = lax.rem(me + k, n)
            pltpu.make_async_remote_copy(
                src_ref=src_of(peer),
                dst_ref=buf.at[me],
                send_sem=ssem.at[phase, peer],
                recv_sem=rsem.at[phase, me],
                device_id={"ep": peer},
                device_id_type=MESH,
            ).start()
            return c

        lax.fori_loop(1, n, body, 0)

    def recv_all(phase, src_of, buf):
        def body(k, c):
            peer = lax.rem(me + n - k, n)
            remote(phase, src_of(peer), buf.at[peer], peer, peer).wait_recv()
            return c

        lax.fori_loop(1, n, body, 0)

    near = me + 1 - 2 * lax.rem(me, 2)

    def spread_out(phase, src, buf):
        def push(peer):
            pltpu.make_async_remote_copy(
                src_ref=src,
                dst_ref=buf.at[me],
                send_sem=ssem.at[phase, peer],
                recv_sem=rsem.at[phase, me],
                device_id={"ep": peer},
                device_id_type=MESH,
            ).start()

        def body(k, c):
            push(lax.rem(me + 2 * k, n))
            return c

        lax.fori_loop(1, n // 2, body, 0)
        push(near)

    def relay(phase, src, buf):
        def body(k, c):
            s = lax.rem(me + n - 2 * k, n)
            remote(phase, src, buf.at[s], s, s).wait_recv()
            pltpu.make_async_remote_copy(
                src_ref=buf.at[s],
                dst_ref=buf.at[s],
                send_sem=ssem.at[phase, s + 1 - 2 * lax.rem(s, 2)],
                recv_sem=rsem.at[phase, s],
                device_id={"ep": near},
                device_id_type=MESH,
            ).start()
            return c

        lax.fori_loop(1, n // 2, body, 0)

    def relayed(phase, src, buf):
        def body(k, c):
            s = lax.rem(near + 2 * k, n)
            remote(phase, src, buf.at[s], s, s).wait_recv()
            return c

        lax.fori_loop(0, n // 2, body, 0)

    def drain(phase, src_of, buf):
        def body(k, c):
            peer = lax.rem(me + k, n)
            remote(phase, src_of(peer), buf.at[peer], peer, peer).wait_send()
            return c

        lax.fori_loop(1, n, body, 0)

    fills[0].wait()
    pl.semaphore_wait(barrier, n - 1)

    whole1 = lambda peer: tok_ref
    spread_out(0, tok_ref, buf1)
    buf1[me] = tok_ref[...]
    for fill in fills[1:]:
        fill.wait()

    own = tok_ref[...].astype(F32)
    own_normed = (
        own * lax.rsqrt(jnp.mean(own * own, axis=-1, keepdims=True) + 1e-06) * mixg_ref[...]
    ).astype(BF16)
    loads[0].wait()
    pre = dot_t(own_normed, wstep[...]) + sbias_ref[...]
    step = jnp.maximum(pre, 0.0) + jnp.log1p(jnp.exp(-jnp.abs(pre)))
    decay = jnp.exp(-step * jnp.exp(dlog_ref[...]))
    small[...] = jnp.zeros_like(small)
    small[0:seq, 0:heads] = step
    small[seq : 2 * seq, 0:heads] = decay
    small[2 * seq : 2 * seq + 1, 0:heads] = skip_ref[...]
    turned = jnp.transpose(small[...])
    for b in range(seq):
        step_b[b] = jnp.broadcast_to(turned[0:heads, b : b + 1], (heads, NSTATE))
        decay_b[b] = jnp.broadcast_to(
            turned[0:heads, seq + b : seq + b + 1], (heads, NSTATE)
        )
    rows_b = jnp.broadcast_to(turned[0:heads, 2 * seq : 2 * seq + 1], (heads, NSTATE))
    per = 128 // hdim
    lane = lax.broadcasted_iota(jnp.int32, (1, 128), 1)

    def spread(value, dst, at):
        for r in range(inner // 128):
            row = value[per * r : per * r + 1]
            for j in range(1, per):
                row = jnp.where(lane < j * hdim, row, value[per * r + j : per * r + j + 1])
            dst[at : at + 1, 128 * r : 128 * r + 128] = row

    spread(rows_b, skip_x, 0)
    for b in range(seq):
        spread(step_b[b], step_x, b)
        spread(decay_b[b], decay_x, b)
    relay(0, tok_ref, buf1)
    taps = cx_ref.shape[0]
    for state_ref, weight_ref, sum_ref, new_ref in (
        (cx_ref, cxw_ref, convx, ncx_ref),
        (cb_ref, cbw_ref, convbc, ncb_ref),
    ):
        total = state_ref[0].astype(F32) * weight_ref[0:1, :]
        for i in range(1, taps):
            new_ref[i - 1] = state_ref[i]
            total = total + state_ref[i].astype(F32) * weight_ref[i : i + 1, :]
        sum_ref[...] = total

    relayed(0, tok_ref, buf1)
    for s in range(n):
        toks[seq * s : seq * s + seq, :] = buf1[s].astype(F32)
    t = toks[...]
    scale = lax.rsqrt(jnp.mean(t * t, axis=-1, keepdims=True) + 1e-06)
    lhs[...] = (toks[...] * scale * mixg_ref[...]).astype(BF16)
    loads[1].wait()
    proj[:, 0:zw] = dot(lhs[...], wz[...])
    loads[2].wait()
    proj[:, zw : zw + xw] = dot(lhs[...], wv[...])
    loads[3].wait()
    proj[:, zw + xw : zw + xw + bw] = dot_t(lhs[...], wbc[...])
    for s in range(n):
        send2[s] = proj[seq * s : seq * s + seq, :].astype(BF16)
    slot2 = lambda peer: send2.at[peer]
    send_all(1, slot2, buf2)
    buf2[me] = send2[me]
    loads[4].wait()

    def narrow(g, c):
        hs = pl.ds(pl.multiple_of(g * hgroup, hgroup), hgroup)
        for b in range(seq):
            state16[b, g] = state[b, hs].reshape(hgroup * hdim, NSTATE).astype(BF16)
        return c

    lax.fori_loop(0, GROUPS, narrow, 0)
    recv_all(1, slot2, buf2)
    for s in range(n):
        zrow[:, zw * s : zw * s + zw] = buf2[s, :, 0:zw].astype(F32)
        ncx_ref[taps - 1, :, xw * s : xw * s + xw] = buf2[s, :, zw : zw + xw]
        ncb_ref[taps - 1, :, bw * s : bw * s + bw] = buf2[s, :, zw + xw : zw + xw + bw]

    xconv[...] = silu(convx[...] + ncx_ref[taps - 1].astype(F32) * cxw_ref[taps : taps + 1, :])
    bcconv[...] = silu(convbc[...] + ncb_ref[taps - 1].astype(F32) * cbw_ref[taps : taps + 1, :])
    gw = hgroup * hdim
    for g in range(GROUPS):
        at = slice(g * gw, g * gw + gw)
        for b in range(seq):
            in_map = bcconv[b : b + 1, g * NSTATE : (g + 1) * NSTATE]
            out_map = bcconv[b : b + 1, (GROUPS + g) * NSTATE : (GROUPS + g + 1) * NSTATE]
            meet = jnp.sum(in_map * out_map, axis=1, keepdims=True)
            left = jnp.broadcast_to(out_map, (8, NSTATE)).astype(BF16)
            y = dot_t(left, state16[b, g])
            yrow[b : b + 1, at] = (
                decay_x[b : b + 1, at] * y[0:1]
                + (meet * step_x[b : b + 1, at] + skip_x[:, at]) * xconv[b : b + 1, at]
            )
    gated = yrow[...] * silu(zrow[...])
    mixed = (
        gated
        * lax.rsqrt(jnp.mean(gated * gated, axis=-1, keepdims=True) + 1e-06)
        * innerg_ref[...]
    ).astype(BF16)
    send3[...] = mixed
    whole3 = lambda peer: send3
    spread_out(2, send3, buf3)
    buf3[me] = mixed
    chunks = hgroup // per
    for g in range(GROUPS):
        for r in range(chunks):
            at = 128 * (chunks * g + r)
            xs[g, seq * r : seq * r + seq, :] = xconv[:, at : at + 128]

    def group(g, c):
        cols = jnp.transpose(xs[g])
        hs = pl.ds(pl.multiple_of(g * hgroup, hgroup), hgroup)
        for b in range(seq):
            at = pl.multiple_of(g * NSTATE, NSTATE)
            ins = step_b[b, hs, :] * bcconv[b : b + 1, pl.ds(at, NSTATE)]
            decs = decay_b[b, hs, :]
            for h in range(hgroup):
                r, j = h // per, h % per
                col = cols[hdim * j : hdim * j + hdim, seq * r + b : seq * r + b + 1]
                nstate_ref[b, g * hgroup + h] = (
                    decs[h : h + 1] * state[b, g * hgroup + h] + col * ins[h : h + 1]
                )
        return c

    lax.fori_loop(0, GROUPS // 2, group, 0)
    relay(2, send3, buf3)
    lax.fori_loop(GROUPS // 2, GROUPS, group, 0)
    relayed(2, send3, buf3)
    for s in range(n):
        rows_f[seq * s : seq * s + seq, :] = buf3[s].astype(F32)
    lhs[...] = rows_f[...].astype(BF16)
    loads[5].wait()
    cols_out = dot(lhs[...], wo[...]).astype(BF16)
    send4[...] = cols_out
    whole4 = lambda peer: send4
    spread_out(3, send4, buf4)
    buf4[me] = cols_out
    relay(3, send4, buf4)
    relayed(3, send4, buf4)

    for s in range(n):
        at = slice(ow * s, ow * s + ow)
        rows_f[:, at] = (toks[:, at] + buf4[s].astype(F32)).astype(BF16).astype(F32)
    t = rows_f[...]
    scale = lax.rsqrt(jnp.mean(t * t, axis=-1, keepdims=True) + 1e-06)
    lhs[...] = (rows_f[...] * scale * ffng_ref[...]).astype(BF16)
    for b in range(seq):
        yrow[b : b + 1, :] = rows_f[pl.ds(me * seq + b, 1), :]
    loads[6].wait()
    gate_part = dot(lhs[...], eg[...])
    loads[7].wait()
    up_part = dot(lhs[...], eu[...])
    act = (silu(gate_part) * up_part).astype(BF16)
    loads[8].wait()
    piece = 512
    for i in range(width // piece):
        at = slice(i * piece, i * piece + piece)
        part = dot(act, ed[:, at])
        for s in range(n):
            send5[s, :, at] = part[seq * s : seq * s + seq].astype(BF16)
    slot5 = lambda peer: send5.at[peer]
    send_all(4, slot5, buf5)
    buf5[me] = send5[me]
    drain(0, whole1, buf1)
    drain(1, slot2, buf2)
    drain(2, whole3, buf3)
    drain(3, whole4, buf4)
    recv_all(4, slot5, buf5)
    total = yrow[...]
    for e in range(n):
        w = jnp.sum(jnp.where(routes_ref[...] == e, rw_ref[...], 0.0), axis=1, keepdims=True)
        total = total + w * buf5[e].astype(F32)
    out_ref[...] = total.astype(BF16)
    drain(4, slot5, buf5)


def entry(n, *refs):
    sources, own = refs[:SMALLS], refs[REFS : REFS + SMALLS]
    fills = [
        pltpu.make_async_copy(src, dst, refs[-1].at[i])
        for i, (src, dst) in enumerate(zip(sources, own))
    ]
    kernel(n, fills, *own, *refs[SMALLS:REFS], *refs[REFS + SMALLS : -1])


def hand_over(*refs):
    sem = refs[8]
    moves = [pltpu.make_async_copy(refs[i], refs[4 + i], sem.at[i]) for i in range(4)]
    for move in reversed(moves):
        move.start()
    for move in moves:
        move.wait()


def body(
    tokens_in,
    mix_gain,
    w_gate_z,
    w_value,
    w_in_bc,
    w_step,
    step_bias,
    decay_log,
    skip_gain,
    conv_x_weight,
    conv_bc_weight,
    conv_x_state,
    conv_bc_state,
    ssm_state,
    inner_gain,
    out_weight,
    ffn_gain,
    expert_gate,
    expert_up,
    expert_down,
    routes,
    route_weight,
):
    n = lax.axis_size("ep")
    seq, width = tokens_in.shape
    heads = step_bias.shape[0]
    inner = conv_x_weight.shape[1]
    bcw = conv_bc_weight.shape[1]
    taps = conv_x_state.shape[1]
    zw, xw, bw = w_gate_z.shape[1], w_value.shape[1], w_in_bc.shape[1]
    pw = zw + xw + bw
    ow = out_weight.shape[1]
    batch = n * seq
    vmem = pl.BlockSpec(memory_space=pltpu.VMEM)
    hbm = pl.BlockSpec(memory_space=pltpu.HBM)
    chunk_rows = heads // GROUPS * (inner // heads) // 128 * seq
    scratch = [
        pltpu.VMEM(w_gate_z.shape, BF16),
        pltpu.VMEM(w_value.shape, BF16),
        pltpu.VMEM(w_in_bc.shape[::-1], BF16),
        pltpu.VMEM(w_step.shape[::-1], BF16),
        pltpu.VMEM(ssm_state.shape, F32),
        pltpu.VMEM(out_weight.shape, BF16),
        pltpu.VMEM(expert_gate.shape[1:], BF16),
        pltpu.VMEM(expert_up.shape[1:], BF16),
        pltpu.VMEM(expert_down.shape[1:], BF16),
        pltpu.VMEM((n, seq, width), BF16),
        pltpu.VMEM((n, seq, pw), BF16),
        pltpu.VMEM((n, seq, pw), BF16),
        pltpu.VMEM((seq, inner), BF16),
        pltpu.VMEM((n, seq, inner), BF16),
        pltpu.VMEM((batch, ow), BF16),
        pltpu.VMEM((n, batch, ow), BF16),
        pltpu.VMEM((n, seq, width), BF16),
        pltpu.VMEM((n, seq, width), BF16),
        pltpu.VMEM((batch, width), F32),
        pltpu.VMEM((batch, width), BF16),
        pltpu.VMEM((batch, pw), F32),
        pltpu.VMEM((128, 128), F32),
        pltpu.VMEM((seq, heads, NSTATE), F32),
        pltpu.VMEM((seq, heads, NSTATE), F32),
        pltpu.VMEM((1, inner), F32),
        pltpu.VMEM((seq, inner), F32),
        pltpu.VMEM((seq, inner), F32),
        pltpu.VMEM((seq, GROUPS, inner // GROUPS, NSTATE), BF16),
        pltpu.VMEM((seq, inner), F32),
        pltpu.VMEM((seq, bcw), F32),
        pltpu.VMEM((seq, inner), F32),
        pltpu.VMEM((seq, bcw), F32),
        pltpu.VMEM((seq, inner), F32),
        pltpu.VMEM((GROUPS, chunk_rows, 128), F32),
        pltpu.VMEM((seq, inner), F32),
        pltpu.VMEM((batch, width), F32),
        pltpu.SemaphoreType.DMA((9,)),
        pltpu.SemaphoreType.DMA((5, n)),
        pltpu.SemaphoreType.DMA((5, n)),
    ]
    operands = (
        tokens_in,
        mix_gain[None, :],
        step_bias[None, :],
        decay_log[None, :],
        skip_gain[None, :],
        conv_x_weight,
        conv_bc_weight,
        jnp.transpose(conv_x_state, (1, 0, 2)),
        jnp.transpose(conv_bc_state, (1, 0, 2)),
        inner_gain[None, :],
        ffn_gain[None, :],
        routes,
        route_weight,
        w_gate_z,
        w_value,
        w_in_bc.T,
        w_step.T,
        ssm_state,
        out_weight,
        expert_gate,
        expert_up,
        expert_down,
    )
    results = pl.pallas_call(
        functools.partial(entry, n),
        out_shape=(
            jax.ShapeDtypeStruct((seq, width), BF16),
            jax.ShapeDtypeStruct((taps, seq, inner), BF16),
            jax.ShapeDtypeStruct((taps, seq, bcw), BF16),
            pltpu.VMEM(ssm_state.shape, F32),
        ),
        in_specs=[hbm] * len(operands),
        out_specs=(vmem, vmem, vmem, vmem),
        scratch_shapes=[pltpu.VMEM(v.shape, v.dtype) for v in operands[:SMALLS]]
        + scratch
        + [pltpu.SemaphoreType.DMA((SMALLS,))],
        compiler_params=pltpu.CompilerParams(
            collective_id=0, has_side_effects=True, vmem_limit_bytes=44 * 1024 * 1024
        ),
    )(*(pltpu.with_memory_space_constraint(v, pltpu.HBM) for v in operands))
    out_tokens, new_x, new_bc, new_state = pl.pallas_call(
        hand_over,
        out_shape=tuple(jax.ShapeDtypeStruct(r.shape, r.dtype) for r in results),
        in_specs=[vmem] * 4,
        out_specs=(hbm,) * 4,
        scratch_shapes=[pltpu.SemaphoreType.DMA((4,))],
        compiler_params=pltpu.CompilerParams(vmem_limit_bytes=8 * 1024 * 1024),
    )(*results)
    return (
        out_tokens,
        new_state,
        jnp.transpose(new_x, (1, 0, 2)),
        jnp.transpose(new_bc, (1, 0, 2)),
    )


def solution(mesh):
    rows = P(("grp", "ep"), None)
    placed = (
        rows,
        P(),
        P(None, "ep"),
        P(None, "ep"),
        P(None, "ep"),
        P(),
        P(),
        P(),
        P(),
        P(),
        P(),
        P(("grp", "ep"), None, None),
        P(("grp", "ep"), None, None),
        P(("grp", "ep"), None, None, None),
        P(),
        P(None, "ep"),
        P(),
        P("ep", None, None),
        P("ep", None, None),
        P("ep", None, None),
        rows,
        rows,
    )
    return jax.shard_map(
        body,
        mesh=mesh,
        in_specs=placed,
        out_specs=(
            rows,
            P(("grp", "ep"), None, None, None),
            P(("grp", "ep"), None, None),
            P(("grp", "ep"), None, None),
        ),
        check_vma=False,
    )
```
